256 devices in a mesh: sp: 16 (over y, x), tp: 16 (over z, core).
Axes of the slice: x: 4, y: 4, z: 8, core: 2. Of those that a mesh axis runs over, the one named last changes fastest.
Arguments:
- saved_input: bfloat16 [4096, 2048], P('sp'), may hold values from -6 to 6
- cotangent: bfloat16 [4096, 2048], P('sp'), may hold values from -6 to 6
- expert_ids: int32 [4096, 2], P('sp'), may hold values from 0 to 15, all different within a row; in each aligned block of 256 rows (0 to 255, 256 to 511, ...) at most 64 rows name the same one
- route_weight: float32 [4096, 2], P('sp'), may hold values from 0.1 to 0.9
- w_gate: bfloat16 [16, 2048, 6144], P('sp', None, 'tp'), may hold values from -0.125 to 0.125
- w_up: bfloat16 [16, 2048, 6144], P('sp', None, 'tp'), may hold values from -0.125 to 0.125
- w_down: bfloat16 [16, 6144, 2048], P('sp', 'tp'), may hold values from -0.078125 to 0.078125
- w_out: bfloat16 [2048, 2048], P(None, 'tp'), may hold values from -0.125 to 0.125
- channel_gain: float32 [2048], P('tp'), may hold values from 0.1 to 1.9
- conv_taps: float32 [31, 2048], P(None, 'tp'), may hold values from -1 to 1
- glu_value: bfloat16 [2048, 4096], P('tp', 'sp'), may hold values from -6 to 6
- glu_gate: bfloat16 [2048, 4096], P('tp', 'sp'), may hold values from -8 to 8
- conv_out: bfloat16 [2048, 4096], P('tp', 'sp'), may hold values from -6 to 6
- norm_mean: float32 [4096], P('sp'), may hold values from -3 to 3
- norm_rstd: float32 [4096], P('sp'), may hold values from 0.5 to 2
Outputs:
- gate_grad: bfloat16 [16, 2048, 6144], P('sp', None, 'tp')
- up_grad: bfloat16 [16, 2048, 6144], P('sp', None, 'tp')
- down_grad: bfloat16 [16, 6144, 2048], P('sp', 'tp')
- proj_grad: float32 [2048, 2048], P('sp', 'tp')
- value_grad: bfloat16 [2048, 4096], P('tp', 'sp')
- gate_in_grad: bfloat16 [2048, 4096], P('tp', 'sp')
The draws below stay inside these ranges and needn't reach their ends.
Inputs may be any that keep to these rules, and one draw needn't show every extreme that they name: `expert_ids`: the two experts of a position differ. In the positions of one block of 256, no expert is named more than 64 times, a bound that some block reaches.
All inputs are finite; a program needn't handle non-finite values.
Results may differ from the reference program's by a relative error of at most 0.018.
Values may be sent and summed in bfloat16 or wider, within the bound.
No kernel may reach another device: no remote copies, remote signals or barrier semaphores. Data moves between devices by JAX's collectives and lax.ppermute only.
A program may use at most 128 MiB of HBM per device.

```python
import math
import jax
import jax.numpy as jnp
import numpy as np
from jax import lax

D = 2048
C = 2048
FF = 6144
CONV_K = 31
TOK_SP = 256
EXPERTS = 16
TOKENS = 4096
CAP = 64
N_SP = 16


def strengthened(drawn, key, source, target, blocks, factor):
    owner, partner = [(jnp.arange(drawn.shape[dim]) // (drawn.shape[dim] // blocks)).reshape([-1 if axis == dim else 1 for axis in range(drawn.ndim)]) for dim in (source, target)]
    chosen = jax.random.permutation(key, blocks)[partner]
    strong = (owner == chosen) | (owner == (partner + blocks // 2) % blocks)
    return jnp.where(strong, factor * drawn, drawn)


def levels(stream_key, dims, split, least, high):
    level = 1.0
    for position, blocks in split:
        heights = jax.random.uniform(jax.random.fold_in(jax.random.fold_in(stream_key, 6), position), (blocks,), jnp.float32, least / len(split), high / len(split))
        level = level * jnp.repeat(jnp.exp(heights), dims[position] // blocks).reshape((-1,) + (1,) * (len(dims) - 1 - position))
    return level


def shared_out(key, own, number, rows, amount, top, bound, skew):
    sequence = jax.random.permutation(key, amount)
    crowded, usual = portions_of(amount, rows * top, bound, skew, True), portions_of(amount, rows * top, bound, skew, False)
    places = jnp.arange(amount)

    def named(tallies, rotation):
        used = int((tallies > 0).sum())
        fixed = max(1, used // 4)
        shifted = fixed + (places - fixed + rotation * (used - fixed)) % max(1, amount - fixed)
        return jnp.zeros((amount,), jnp.int32).at[sequence[jnp.where(places < fixed, places, shifted)]].set(jnp.asarray(tallies, jnp.int32))

    tallies = jnp.where(number % 4 == 0, named(crowded, number // 4), named(usual, number - number // 4 - 1))
    mixed = jax.random.permutation(jax.random.fold_in(own, 3), amount)
    giver, taker = mixed[0:amount // 2 * 2:2], mixed[1:amount // 2 * 2:2]
    room = jnp.minimum(tallies[giver] - 1, bound - tallies[taker]) // 2
    room = jnp.where((giver == sequence[0]) | (taker == sequence[0]) | (tallies[taker] == 0), 0, jnp.maximum(room, 0))
    shifted = jax.random.randint(jax.random.fold_in(own, 4), (amount // 2,), 0, 1 << 20) % (room + 1)
    tallies = tallies.at[giver].add(-shifted).at[taker].add(shifted)
    items = jnp.searchsorted(jnp.cumsum(tallies), jnp.arange(rows * top), side="right").astype(jnp.int32)
    grid = items.reshape(top, rows).T
    grid = grid[jax.random.permutation(jax.random.fold_in(own, 1), rows)]
    rotation = jax.random.randint(jax.random.fold_in(own, 2), (rows, 1), 0, top)
    return jnp.take_along_axis(grid, (jnp.arange(top)[None, :] + rotation) % top, axis=1)


def portions_of(number_of, total, most, lean, full):
    loads = [(1 << 20) // math.isqrt(standing ** lean) + 1 for standing in range(1, number_of + 1)]
    largest = most if full else min(most, max(-(-total // number_of), total * loads[0] // sum(loads)))
    least = 1 if total - largest >= number_of - 1 else 0
    given, rest = [largest] + [least] * (number_of - 1), total - largest - least * (number_of - 1)
    while rest > 0:
        movable = [i for i in range(1, number_of) if given[i] < largest] or [i for i in range(1, number_of) if given[i] < most]
        whole, budget = sum([loads[i] for i in movable]), rest
        for i in movable:
            addition = min(most - given[i], max(1, budget * loads[i] // whole), rest)
            given[i] = given[i] + addition
            rest = rest - addition
    return np.array(given)


def gaussian(stream_key, dims, deviation, reach, pieces=(), held_as=jnp.bfloat16):
    factor_of = levels(stream_key, dims, pieces, -0.22, 0.18) if pieces else 1.0
    result = jax.random.normal(stream_key, dims, jnp.float32) * deviation * factor_of
    return jnp.minimum(jnp.maximum(result, -reach), reach).astype(held_as)


def bell_draw_with(key, extent, scale, reach, shards, heavy, held_as=jnp.bfloat16):
    drawn = scale * jax.random.normal(key, extent, jnp.float32)
    if shards:
        drawn = drawn * levels(key, extent, shards, -0.22, 0.18)
    return jnp.clip(strengthened(drawn, jax.random.fold_in(key, 3), *heavy), -reach, reach).astype(held_as)


def setup_inputs(seed: int = 0) -> dict:
    key_list = jax.random.split(jax.random.key(seed), 16)
    saved_input = gaussian(key_list[0], (TOKENS, D), 1.0, 6.0, ((0, 16),))
    cotangent = bell_draw_with(key_list[1], (TOKENS, D), 1.0, 6.0, ((0, 16),), (0, 1, 16, 2.0))
    expert_ids_keys = jax.random.split(jax.random.fold_in(key_list[2], 1), TOKENS // TOK_SP)
    expert_ids_turns = jax.random.permutation(jax.random.fold_in(key_list[2], 3), TOKENS // TOK_SP)
    expert_ids = jax.vmap(lambda own, number: shared_out(jax.random.fold_in(key_list[2], 2), own, number, TOK_SP, EXPERTS, 2, CAP, 1))(expert_ids_keys, expert_ids_turns).reshape((TOKENS, 2))
    route_weight = jnp.clip(0.1 + 0.79999997 * jax.random.uniform(key_list[3], (TOKENS, 2), jnp.float32) ** levels(key_list[3], (TOKENS, 2), ((0, 16),), -0.2, 0.2), 0.1, 0.9)
    w_gate = gaussian(key_list[4], (EXPERTS, D, FF), D ** -0.5, 0.125, ((0, 16), (2, 16)))
    w_up = gaussian(key_list[5], (EXPERTS, D, FF), D ** -0.5, 0.125, ((0, 16), (2, 16)))
    w_down = gaussian(key_list[6], (EXPERTS, FF, D), FF ** -0.5, 0.078125, ((0, 16), (1, 16)))
    w_out = gaussian(key_list[7], (D, C), C ** -0.5, 0.125, ((1, 16),))
    channel_gain = jnp.clip(1.0 + 0.18 * jax.random.normal(key_list[8], (C,), jnp.float32), 0.1, 1.9)
    conv_taps = gaussian(key_list[9], (CONV_K, C), CONV_K ** -0.5, 1.0, ((1, 16),), jnp.float32)
    glu_value = gaussian(key_list[10], (C, TOKENS), 1.0, 6.0, ((0, 16), (1, 16)))
    glu_gate = gaussian(key_list[11], (C, TOKENS), 1.5, 8.0, ((0, 16), (1, 16)))
    conv_out = gaussian(key_list[12], (C, TOKENS), 1.0, 6.0, ((0, 16), (1, 16)))
    norm_mean = gaussian(key_list[13], (TOKENS,), 0.5, 3.0, ((0, 16),), jnp.float32)
    norm_rstd = jnp.clip(jnp.exp(math.log(2.0) - 1.3862944 * jax.random.uniform(key_list[14], (TOKENS,), jnp.float32) ** levels(key_list[14], (TOKENS,), ((0, 16),), -0.2, 0.2)), 0.5, 2.0)
    return dict(saved_input=saved_input, cotangent=cotangent, expert_ids=expert_ids, route_weight=route_weight, w_gate=w_gate, w_up=w_up, w_down=w_down, w_out=w_out, channel_gain=channel_gain, conv_taps=conv_taps, glu_value=glu_value, glu_gate=glu_gate, conv_out=conv_out, norm_mean=norm_mean, norm_rstd=norm_rstd)


def contract(left, right, left_dim, right_dim):
    return lax.dot_general(left, right, (((left_dim,), (right_dim,)), ((), ())), preferred_element_type=jnp.float32)


def expert_grads(rows_in, rows_cot, gate_weight, up_weight, down_weight):
    gate_pre = jnp.dot(rows_in, gate_weight, preferred_element_type=jnp.float32)
    up_pre = jnp.dot(rows_in, up_weight, preferred_element_type=jnp.float32)
    sigma = jax.nn.sigmoid(gate_pre)
    hidden = (gate_pre * sigma * up_pre).astype(jnp.bfloat16)
    hidden_cot = contract(rows_cot, down_weight, 1, 1)
    down_part = contract(hidden, rows_cot, 0, 0).astype(jnp.bfloat16)
    gate_cot = (hidden_cot * up_pre * sigma * (1.0 + gate_pre * (1.0 - sigma))).astype(jnp.bfloat16)
    up_cot = (hidden_cot * gate_pre * sigma).astype(jnp.bfloat16)
    gate_part = contract(rows_in, gate_cot, 0, 0).astype(jnp.bfloat16)
    up_part = contract(rows_in, up_cot, 0, 0).astype(jnp.bfloat16)
    input_cot = contract(gate_cot, gate_weight, 1, 1) + contract(up_cot, up_weight, 1, 1)
    return gate_part, up_part, down_part, input_cot


def reference(saved_input, cotangent, expert_ids, route_weight, w_gate, w_up, w_down, w_out,
              channel_gain, conv_taps, glu_value, glu_gate, conv_out, norm_mean, norm_rstd):
    pairs = expert_ids.reshape(N_SP, 2 * TOK_SP)
    onehot = (pairs[:, :, None] == jnp.arange(EXPERTS, dtype=jnp.int32)[None, None, :]).astype(jnp.int32)
    before = jnp.cumsum(onehot, axis=1) - onehot
    slots = jnp.sum(before * onehot, axis=2)
    source = jnp.arange(N_SP, dtype=jnp.int32)[:, None]
    target = (pairs * (N_SP * CAP) + source * CAP + slots).reshape(2 * TOKENS).astype(jnp.int32)
    owner = jnp.zeros((EXPERTS * N_SP * CAP,), jnp.int32).at[target].set(jnp.arange(2 * TOKENS, dtype=jnp.int32) + 1)
    filled = (owner > 0)[:, None]
    pair_index = jnp.maximum(owner - 1, 0)
    scaled = (route_weight[:, :, None] * cotangent.astype(jnp.float32)[:, None, :]).astype(jnp.bfloat16)
    scaled = scaled.reshape(2 * TOKENS, D)
    rows_cot = jnp.where(filled, scaled[pair_index], jnp.zeros_like(scaled[:1])).reshape(EXPERTS, N_SP * CAP, D)
    rows_in = jnp.where(filled, saved_input[pair_index // 2], jnp.zeros_like(saved_input[:1]))
    rows_in = rows_in.reshape(EXPERTS, N_SP * CAP, D)
    gate_grad, up_grad, down_grad, input_cot = lax.map(
        lambda packed: expert_grads(*packed), (rows_in, rows_cot, w_gate, w_up, w_down))
    routed = input_cot.reshape(EXPERTS * N_SP * CAP, D)[target].reshape(TOKENS, 2, D)
    mixed_cot = (cotangent.astype(jnp.float32) + jnp.sum(routed, axis=1)).astype(jnp.bfloat16)

    centered = (conv_out.astype(jnp.float32) - norm_mean[None, :]) * norm_rstd[None, :]
    normed = centered * channel_gain[:, None]
    sigma = jax.nn.sigmoid(normed)
    output_act = (normed * sigma).astype(jnp.bfloat16)
    proj_grad = contract(mixed_cot, output_act, 0, 1)
    act_cot = contract(w_out, mixed_cot, 0, 1)
    norm_cot = act_cot * sigma * (1.0 + normed * (1.0 - sigma)) * channel_gain[:, None]
    first_sum = jnp.sum(norm_cot, axis=0)
    second_sum = jnp.sum(norm_cot * centered, axis=0)
    conv_cot = norm_rstd[None, :] * (norm_cot - first_sum[None, :] / C - centered * second_sum[None, :] / C)
    padded = jnp.pad(conv_cot, ((0, 0), (0, CONV_K - 1)))
    glu_cot = conv_taps[0][:, None] * padded[:, :TOKENS]
    for lag in range(1, CONV_K):
        glu_cot = glu_cot + conv_taps[lag][:, None] * padded[:, lag:lag + TOKENS]
    gate_sigma = jax.nn.sigmoid(glu_gate.astype(jnp.float32))
    value_grad = (glu_cot * gate_sigma).astype(jnp.bfloat16)
    gate_in_grad = (glu_cot * glu_value.astype(jnp.float32) * gate_sigma * (1.0 - gate_sigma)).astype(jnp.bfloat16)
    return gate_grad, up_grad, down_grad, proj_grad, value_grad, gate_in_grad
```

```python
import functools

import jax
import jax.numpy as jnp
from jax import lax
from jax.experimental import pallas as pl
from jax.experimental.pallas import tpu as pltpu
from jax.sharding import PartitionSpec as P

D = 2048
C = 2048
HALF = D // 2
BF = jnp.bfloat16
F32 = jnp.float32


def contract(left, right, left_dim, right_dim):
    return lax.dot_general(
        left, right, (((left_dim,), (right_dim,)), ((), ())), preferred_element_type=F32
    )


def exchanged(value, axis, groups=None):
    return lax.all_to_all(value, axis, 0, 0, axis_index_groups=groups, tiled=True)


def swapped_cores(value):
    pairs = [(i, i ^ 1) for i in range(lax.axis_size("tp"))]
    return lax.ppermute(value, "tp", pairs)


def route_kernel(core, ids, weights, rows_in, rows_cot, sent, target, *, experts, slots):
    tokens = ids.shape[1]
    step = pl.program_id(0)
    rows = sent.shape[0]

    @pl.when(step == 0)
    def _():
        expert = lax.broadcasted_iota(jnp.int32, (experts, tokens), 0)
        first = ids[0:1, :] == expert
        second = ids[1:2, :] == expert
        named = jnp.where(first | second, 1.0, 0.0).astype(BF)
        earlier = lax.broadcasted_iota(jnp.int32, (tokens, tokens), 0) < lax.broadcasted_iota(
            jnp.int32, (tokens, tokens), 1
        )
        count = jnp.dot(named, jnp.where(earlier, 1.0, 0.0).astype(BF), preferred_element_type=F32)
        for k, chosen in ((0, first), (1, second)):
            slot = jnp.sum(jnp.where(chosen, count, 0.0), axis=0, keepdims=True)
            target[k : k + 1, :] = ids[k : k + 1, :] * slots + slot.astype(jnp.int32)

    row = lax.broadcasted_iota(jnp.int32, (rows, tokens), 0) + step * rows
    hit0 = row == target[0:1, :]
    hit1 = row == target[1:2, :]
    select = jnp.where(hit0 | hit1, 1.0, 0.0).astype(BF)
    weight = jnp.sum(
        jnp.where(hit0, weights[0:1, :], 0.0) + jnp.where(hit1, weights[1:2, :], 0.0),
        axis=1,
        keepdims=True,
    )
    width = rows_in.shape[1]
    sent[:, :width] = jnp.dot(select, rows_in[...], preferred_element_type=F32).astype(BF)
    moved = jnp.dot(select, rows_cot[...], preferred_element_type=F32)
    sent[:, width:] = (moved * weight).astype(BF)


def routed(core, ids, weights, saved_input, cotangent, experts, slots):
    tokens = ids.shape[1]
    rows = 256
    return pl.pallas_call(
        functools.partial(route_kernel, experts=experts, slots=slots),
        grid_spec=pltpu.PrefetchScalarGridSpec(
            num_scalar_prefetch=1,
            grid=(experts * slots // rows,),
            in_specs=[
                pl.BlockSpec((2, tokens), lambda i, c: (0, 0)),
                pl.BlockSpec((2, tokens), lambda i, c: (0, 0)),
                pl.BlockSpec((tokens, HALF), lambda i, c: (0, c[0])),
                pl.BlockSpec((tokens, HALF), lambda i, c: (0, c[0])),
            ],
            out_specs=[
                pl.BlockSpec((rows, D), lambda i, c: (i, 0)),
                pl.BlockSpec((2, tokens), lambda i, c: (0, 0)),
            ],
        ),
        out_shape=[
            jax.ShapeDtypeStruct((experts * slots, D), BF),
            jax.ShapeDtypeStruct((2, tokens), jnp.int32),
        ],
        name="route",
    )(core, ids, weights, saved_input, cotangent)


def expert_kernel(
    core, own, other, gate_own, gate_other, up_own, up_other, down_own, down_other,
    hidden_out, gate_out, up_out, keep, send,
):
    own_in, own_cot = own[:, :HALF], own[:, HALF:]
    other_in, other_cot = other[:, :HALF], other[:, HALF:]
    gate_pre = contract(own_in, gate_own[...], 1, 0) + contract(other_in, gate_other[...], 1, 0)
    up_pre = contract(own_in, up_own[...], 1, 0) + contract(other_in, up_other[...], 1, 0)
    hidden_cot = contract(own_cot, down_own[...], 1, 1) + contract(other_cot, down_other[...], 1, 1)
    sigma = jax.nn.sigmoid(gate_pre)
    silu = gate_pre * sigma
    hidden_out[...] = (silu * up_pre).astype(BF)
    gate_cot = (hidden_cot * up_pre * sigma * (1.0 + gate_pre * (1.0 - sigma))).astype(BF)
    up_cot = (hidden_cot * silu).astype(BF)
    gate_out[...] = gate_cot
    up_out[...] = up_cot
    send[...] = (
        contract(gate_cot, gate_other[...], 1, 1) + contract(up_cot, up_other[...], 1, 1)
    ).astype(BF)
    keep[...] = (
        contract(gate_cot, gate_own[...], 1, 1) + contract(up_cot, up_own[...], 1, 1)
    ).astype(BF)


def expert_pass(core, own, other, w_gate, w_up, w_down):
    total = own.shape[0]
    units = w_gate.shape[1]
    rows = 256
    row_block = lambda width: pl.BlockSpec((rows, width), lambda i, c: (i, 0))
    in_half = lambda flip: pl.BlockSpec(
        (HALF, units), (lambda i, c: (1 - c[0], 0)) if flip else (lambda i, c: (c[0], 0))
    )
    out_half = lambda flip: pl.BlockSpec(
        (units, HALF), (lambda i, c: (0, 1 - c[0])) if flip else (lambda i, c: (0, c[0]))
    )
    return pl.pallas_call(
        expert_kernel,
        grid_spec=pltpu.PrefetchScalarGridSpec(
            num_scalar_prefetch=1,
            grid=(total // rows,),
            in_specs=[
                row_block(D),
                row_block(D),
                in_half(False),
                in_half(True),
                in_half(False),
                in_half(True),
                out_half(False),
                out_half(True),
            ],
            out_specs=[
                row_block(units),
                row_block(units),
                row_block(units),
                row_block(HALF),
                row_block(HALF),
            ],
        ),
        out_shape=[
            jax.ShapeDtypeStruct((total, units), BF),
            jax.ShapeDtypeStruct((total, units), BF),
            jax.ShapeDtypeStruct((total, units), BF),
            jax.ShapeDtypeStruct((total, HALF), BF),
            jax.ShapeDtypeStruct((total, HALF), BF),
        ],
        name="experts",
    )(core, own, other, w_gate, w_gate, w_up, w_up, w_down, w_down)


def grad_kernel(core, own_in, own_cot, other_in, other_cot, hidden, gate_cot, up_cot,
                gate_grad, up_grad, down_grad, hidden_t):
    step = pl.program_id(0)
    half_steps = pl.num_programs(0) // 2

    @pl.when(step == 0)
    def _():
        hidden_t[...] = hidden[...].T

    def block(rows_in, rows_cot):
        turned = rows_in[...].T
        gate_grad[...] = contract(turned, gate_cot[...], 1, 0).astype(BF)
        up_grad[...] = contract(turned, up_cot[...], 1, 0).astype(BF)
        down_grad[...] = contract(hidden_t[...], rows_cot[...], 1, 0).astype(BF)

    @pl.when(step < half_steps)
    def _():
        block(own_in, own_cot)

    @pl.when(step >= half_steps)
    def _():
        block(other_in, other_cot)


def expert_weight_grads(core, own, other, hidden, gate_cot, up_cot):
    total, units = hidden.shape
    cols = 256
    half_steps = HALF // cols

    def own_spec(offset):
        return pl.BlockSpec(
            (total, cols), lambda i, c: (0, jnp.minimum(i, half_steps - 1) + offset)
        )

    def other_spec(offset):
        return pl.BlockSpec(
            (total, cols), lambda i, c: (0, jnp.maximum(i - half_steps, 0) + offset)
        )

    def place(i, c):
        mine = i < half_steps
        return jnp.where(mine, c[0] * half_steps + i, (1 - c[0]) * half_steps + i - half_steps)

    whole = pl.BlockSpec((total, units), lambda i, c: (0, 0))
    return pl.pallas_call(
        grad_kernel,
        grid_spec=pltpu.PrefetchScalarGridSpec(
            num_scalar_prefetch=1,
            grid=(2 * half_steps,),
            in_specs=[
                own_spec(0),
                own_spec(half_steps),
                other_spec(0),
                other_spec(half_steps),
                whole,
                whole,
                whole,
            ],
            out_specs=[
                pl.BlockSpec((cols, units), lambda i, c: (place(i, c), 0)),
                pl.BlockSpec((cols, units), lambda i, c: (place(i, c), 0)),
                pl.BlockSpec((units, cols), lambda i, c: (0, place(i, c))),
            ],
            scratch_shapes=[pltpu.VMEM((units, total), BF)],
        ),
        out_shape=[
            jax.ShapeDtypeStruct((D, units), BF),
            jax.ShapeDtypeStruct((D, units), BF),
            jax.ShapeDtypeStruct((units, D), BF),
        ],
        name="weight_grads",
    )(core, own, own, other, other, hidden, gate_cot, up_cot)


def combine_kernel(target, rows, out, select):
    tokens = target.shape[0]

    @pl.when(pl.program_id(0) == 0)
    def _():
        row = lax.broadcasted_iota(jnp.int32, (tokens, rows.shape[0]), 1)
        hit = (row == target[:, 0:1]) | (row == target[:, 1:2])
        select[...] = jnp.where(hit, 1.0, 0.0).astype(BF)

    out[...] = jnp.dot(select[...], rows[...], preferred_element_type=F32).astype(BF)[None]


def combined(target, rows):
    tokens = target.shape[0]
    total, width = rows.shape
    cols = 128
    return pl.pallas_call(
        combine_kernel,
        grid=(width // cols,),
        in_specs=[
            pl.BlockSpec((tokens, 2), lambda i: (0, 0)),
            pl.BlockSpec((total, cols), lambda i: (0, i)),
        ],
        out_specs=pl.BlockSpec((1, tokens, cols), lambda i: (i, 0, 0)),
        out_shape=jax.ShapeDtypeStruct((width // cols, tokens, cols), BF),
        scratch_shapes=[pltpu.VMEM((tokens, total), BF)],
        name="combine",
    )(target, rows)


def on_device(
    saved_input,
    cotangent,
    expert_ids,
    route_weight,
    w_gate,
    w_up,
    w_down,
    w_out,
    channel_gain,
    conv_taps,
    glu_value,
    glu_gate,
    conv_out,
    norm_mean,
    norm_rstd,
):
    tokens = cotangent.shape[0]
    sp_count = lax.axis_size("sp")
    experts = sp_count
    slots = 4 * tokens // experts
    tp_index = lax.axis_index("tp")
    core_index = tp_index % 2
    core = core_index.reshape(1).astype(jnp.int32)
    tp_count = lax.axis_size("tp")
    depth = tp_count // 2
    same_core = [[2 * z + c for z in range(depth)] for c in range(2)]
    share = HALF // depth

    sent, target = routed(
        core, expert_ids.T, route_weight.T, saved_input, cotangent, experts, slots
    )
    own = exchanged(sent.reshape(experts, slots, D), "sp").reshape(sp_count * slots, D)
    other = swapped_cores(own)
    hidden, gate_cot, up_cot, keep, send = expert_pass(
        core, own, other, w_gate[0], w_up[0], w_down[0]
    )
    received = swapped_cores(send)
    input_cot = (keep.astype(F32) + received.astype(F32)).astype(BF)
    returned = exchanged(input_cot.reshape(sp_count, slots, HALF), "sp")
    gate_grad, up_grad, down_grad = expert_weight_grads(core, own, other, hidden, gate_cot, up_cot)

    parts = combined(target.T, returned.reshape(experts * slots, HALF))
    pieces = exchanged(parts, "tp", same_core)
    cot_share = lax.dynamic_slice(
        cotangent, (0, core_index * HALF + (tp_index // 2) * share), (tokens, share)
    )
    mixed_share = (
        cot_share.astype(F32) + jnp.sum(pieces.astype(F32), axis=0)
    ).astype(BF)
    mixed_own = exchanged(
        jnp.broadcast_to(mixed_share, (depth, tokens, share)), "tp", same_core
    )
    mixed_other = swapped_cores(mixed_own)
    first = jnp.where(core_index == 0, mixed_own, mixed_other)
    second = jnp.where(core_index == 0, mixed_other, mixed_own)
    mixed = jnp.concatenate([first, second], axis=0)

    centered = (conv_out.astype(F32) - norm_mean[None, :]) * norm_rstd[None, :]
    normed = centered * channel_gain[:, None]
    sigma = jax.nn.sigmoid(normed)
    output_act = (normed * sigma).astype(BF)
    slope = sigma * (1.0 + normed * (1.0 - sigma)) * channel_gain[:, None]

    act_cot = lax.dot_general(
        w_out.reshape(D // share, share, -1),
        mixed,
        (((0, 1), (0, 2)), ((), ())),
        preferred_element_type=F32,
    )
    norm_cot = act_cot * slope
    sums = jnp.stack([jnp.sum(norm_cot, axis=0), jnp.sum(norm_cot * centered, axis=0)])
    sums = jnp.sum(
        exchanged(jnp.broadcast_to(sums, (tp_count, 2, tokens)), "tp"), axis=0
    )
    proj_part = lax.dot_general(
        mixed, output_act, (((1,), (1,)), ((), ())), preferred_element_type=F32
    ).astype(BF)
    proj_grad = jnp.sum(exchanged(proj_part, "sp").astype(F32), axis=0)

    conv_cot = norm_rstd[None, :] * (
        norm_cot - sums[0][None, :] / C - centered * sums[1][None, :] / C
    )
    reach = conv_taps.shape[0] - 1
    rim = lax.ppermute(conv_cot[:, :reach], "sp", [(i, i - 1) for i in range(1, sp_count)])
    padded = jnp.concatenate([conv_cot, rim], axis=1)
    glu_cot = conv_taps[0][:, None] * padded[:, :tokens]
    for lag in range(1, reach + 1):
        glu_cot = glu_cot + conv_taps[lag][:, None] * padded[:, lag : lag + tokens]
    gate_sigma = jax.nn.sigmoid(glu_gate.astype(F32))
    value_grad = (glu_cot * gate_sigma).astype(BF)
    gate_in_grad = (glu_cot * glu_value.astype(F32) * gate_sigma * (1.0 - gate_sigma)).astype(BF)
    return (
        gate_grad[None],
        up_grad[None],
        down_grad[None],
        proj_grad,
        value_grad,
        gate_in_grad,
    )


def solution(mesh):
    in_specs = (
        P("sp", None),
        P("sp", None),
        P("sp", None),
        P("sp", None),
        P("sp", None, "tp"),
        P("sp", None, "tp"),
        P("sp", "tp", None),
        P(None, "tp"),
        P("tp"),
        P(None, "tp"),
        P("tp", "sp"),
        P("tp", "sp"),
        P("tp", "sp"),
        P("sp"),
        P("sp"),
    )
    out_specs = (
        P("sp", None, "tp"),
        P("sp", None, "tp"),
        P("sp", "tp", None),
        P("sp", "tp"),
        P("tp", "sp"),
        P("tp", "sp"),
    )
    return jax.shard_map(
        on_device, mesh=mesh, in_specs=in_specs, out_specs=out_specs, check_vma=False
    )
```

```python
import functools

import jax
import jax.numpy as jnp
from jax import lax
from jax.experimental import pallas as pl
from jax.experimental.pallas import tpu as pltpu
from jax.sharding import PartitionSpec as P


D = 2048
C = 2048
HALF = D // 2
BF = jnp.bfloat16
F32 = jnp.float32


def contract(left, right, left_dim, right_dim):
    return lax.dot_general(
        left, right, (((left_dim,), (right_dim,)), ((), ())), preferred_element_type=F32
    )


def exchanged(value, axis, groups=None):
    return lax.all_to_all(value, axis, 0, 0, axis_index_groups=groups, tiled=True)


def swapped_cores(value):
    pairs = [(i, i ^ 1) for i in range(lax.axis_size("tp"))]
    return lax.ppermute(value, "tp", pairs)


def small_vmem():
    return pltpu.CompilerParams(vmem_limit_bytes=6 * 1024 * 1024)


def in_vmem(count):
    return [pl.BlockSpec(memory_space=pltpu.VMEM)] * count


SCALAR = pl.BlockSpec(memory_space=pltpu.SMEM)


def route_kernel(pairs, saved_input, cotangent, sent, target, *, experts, slots):
    tokens = pairs.shape[1]
    ids = pairs[0:2, :].astype(jnp.int32)
    weights = pairs[2:4, :]
    expert = lax.broadcasted_iota(jnp.int32, (experts, tokens), 0)
    first = ids[0:1, :] == expert
    second = ids[1:2, :] == expert
    named = jnp.where(first | second, 1.0, 0.0).astype(BF)
    earlier = lax.broadcasted_iota(jnp.int32, (tokens, tokens), 0) < lax.broadcasted_iota(
        jnp.int32, (tokens, tokens), 1
    )
    count = jnp.dot(named, jnp.where(earlier, 1.0, 0.0).astype(BF), preferred_element_type=F32)
    places = []
    for k, chosen in ((0, first), (1, second)):
        slot = jnp.sum(jnp.where(chosen, count, 0.0), axis=0, keepdims=True)
        places.append(ids[k : k + 1, :] * slots + slot.astype(jnp.int32))
    across = jnp.concatenate(places + [jnp.zeros((6, tokens), jnp.int32)], axis=0)
    target[...] = across.astype(F32).T[:, 0:2].astype(jnp.int32)

    rows = 256
    for step in range(experts * slots // rows):
        row = lax.broadcasted_iota(jnp.int32, (rows, tokens), 0) + step * rows
        hit0 = row == places[0]
        hit1 = row == places[1]
        select = jnp.where(hit0 | hit1, 1.0, 0.0).astype(BF)
        weight = jnp.sum(
            jnp.where(hit0, weights[0:1, :], 0.0) + jnp.where(hit1, weights[1:2, :], 0.0),
            axis=1,
            keepdims=True,
        )
        here = slice(step * rows, (step + 1) * rows)
        moved_in = jnp.dot(select, saved_input[...], preferred_element_type=F32)
        sent[here, :HALF] = moved_in.astype(BF)
        moved = jnp.dot(select, cotangent[...], preferred_element_type=F32)
        sent[here, HALF:] = (moved * weight).astype(BF)


def routed(pairs, half_in, half_cot, experts, slots):
    tokens = pairs.shape[1]
    return pl.pallas_call(
        functools.partial(route_kernel, experts=experts, slots=slots),
        in_specs=in_vmem(3),
        out_specs=in_vmem(2),
        out_shape=[
            jax.ShapeDtypeStruct((experts * slots, D), BF),
            jax.ShapeDtypeStruct((tokens, 2), jnp.int32),
        ],
        compiler_params=small_vmem(),
        name="route",
    )(pairs, half_in, half_cot)


ROWS = 256


def half_of(core, flip):
    index = 1 - core[0] if flip else core[0]
    return pl.ds(pl.multiple_of(index * HALF, HALF), HALF)


def own_kernel(core, own, w_gate, w_up, w_down, first_part, cot_part, pair_own, pair_other):
    units = w_gate.shape[1]
    half, far = half_of(core, False), half_of(core, True)
    pair_own[:, :units] = w_gate[half, :]
    pair_own[:, units:] = w_up[half, :]
    for step in range(own.shape[0] // ROWS):
        here = slice(step * ROWS, (step + 1) * ROWS)
        first_part[here, :] = contract(own[here, :HALF], pair_own[...], 1, 0)
        cot_part[here, :] = contract(own[here, HALF:], w_down[:, half], 1, 1)
    pair_other[:, :units] = w_gate[far, :]
    pair_other[:, units:] = w_up[far, :]


def own_products(core, own, w_gate, w_up, w_down):
    total, units = own.shape[0], w_gate.shape[1]
    return pl.pallas_call(
        own_kernel,
        in_specs=[SCALAR] + in_vmem(4),
        out_specs=in_vmem(4),
        out_shape=[
            jax.ShapeDtypeStruct((total, 2 * units), F32),
            jax.ShapeDtypeStruct((total, units), F32),
            jax.ShapeDtypeStruct((HALF, 2 * units), BF),
            jax.ShapeDtypeStruct((HALF, 2 * units), BF),
        ],
        compiler_params=small_vmem(),
        name="own_products",
    )(core, own, w_gate, w_up, w_down)


def other_kernel(
    core, other, first_part, cot_part, pair_other, w_down, hidden_out, cots, send,
):
    half = half_of(core, True)
    units = w_down.shape[0]
    for step in range(other.shape[0] // ROWS):
        here = slice(step * ROWS, (step + 1) * ROWS)
        first = first_part[here, :] + contract(other[here, :HALF], pair_other[...], 1, 0)
        gate_pre, up_pre = first[:, :units], first[:, units:]
        hidden_cot = cot_part[here, :] + contract(other[here, HALF:], w_down[:, half], 1, 1)
        sigma = jax.nn.sigmoid(gate_pre)
        silu = gate_pre * sigma
        hidden_out[here, :] = (silu * up_pre).astype(BF)
        cots[here, :units] = (
            hidden_cot * up_pre * sigma * (1.0 + gate_pre * (1.0 - sigma))
        ).astype(BF)
        cots[here, units:] = (hidden_cot * silu).astype(BF)
        send[here, :] = contract(cots[here, :], pair_other[...], 1, 1).astype(BF)


def other_products(core, other, first_part, cot_part, pair_other, w_down):
    total, units = other.shape[0], w_down.shape[0]
    return pl.pallas_call(
        other_kernel,
        in_specs=[SCALAR] + in_vmem(5),
        out_specs=in_vmem(3),
        out_shape=[
            jax.ShapeDtypeStruct((total, units), BF),
            jax.ShapeDtypeStruct((total, 2 * units), BF),
            jax.ShapeDtypeStruct((total, HALF), BF),
        ],
        compiler_params=small_vmem(),
        name="other_products",
    )(core, other, first_part, cot_part, pair_other, w_down)


def keep_kernel(cots, pair_own, hidden, keep, hidden_t):
    for step in range(keep.shape[0] // ROWS):
        here = slice(step * ROWS, (step + 1) * ROWS)
        keep[here, :] = contract(cots[here, :], pair_own[...], 1, 1).astype(BF)
    hidden_t[...] = hidden[...].T


def kept_half(cots, pair_own, hidden):
    total, units = hidden.shape
    return pl.pallas_call(
        keep_kernel,
        in_specs=in_vmem(3),
        out_specs=in_vmem(2),
        out_shape=[
            jax.ShapeDtypeStruct((total, HALF), BF),
            jax.ShapeDtypeStruct((units, total), BF),
        ],
        compiler_params=small_vmem(),
        name="kept_half",
    )(cots, pair_own, hidden)


def sum_kernel(keep, received, out):
    out[...] = (keep[...].astype(F32) + received[...].astype(F32)).astype(BF)


def pair_sum(keep, received):
    return pl.pallas_call(
        sum_kernel,
        in_specs=in_vmem(2),
        out_specs=in_vmem(1)[0],
        out_shape=jax.ShapeDtypeStruct(keep.shape, BF),
        compiler_params=small_vmem(),
        name="pair_sum",
    )(keep, received)


def grad_kernel(core, rows_in, rows_cot, hidden_t, cots, *rest):
    gate_grad, up_grad, down_grad = rest[-3:]
    units = gate_grad.shape[1]
    both = contract(rows_in[...].T, cots[...], 1, 0).astype(BF)
    gate_grad[...] = both[:, :units]
    up_grad[...] = both[:, units:]
    down_grad[...] = contract(hidden_t[...], rows_cot[...], 1, 0).astype(BF)


def half_grads(core, flip, rows, hidden_t, cots, before=()):
    units, total = hidden_t.shape
    cols = 256
    steps = HALF // cols

    def place(i, c):
        return (1 - c[0] if flip else c[0]) * steps + i

    return pl.pallas_call(
        grad_kernel,
        grid_spec=pltpu.PrefetchScalarGridSpec(
            num_scalar_prefetch=1,
            grid=(steps,),
            in_specs=[
                pl.BlockSpec((total, cols), lambda i, c: (0, i)),
                pl.BlockSpec((total, cols), lambda i, c: (0, i + steps)),
                pl.BlockSpec((units, total), lambda i, c: (0, 0)),
                pl.BlockSpec((total, 2 * units), lambda i, c: (0, 0)),
            ]
            + [pl.BlockSpec(memory_space=pl.ANY)] * len(before),
            out_specs=[
                pl.BlockSpec((cols, units), lambda i, c: (place(i, c), 0)),
                pl.BlockSpec((cols, units), lambda i, c: (place(i, c), 0)),
                pl.BlockSpec((units, cols), lambda i, c: (0, place(i, c))),
            ],
        ),
        out_shape=[
            jax.ShapeDtypeStruct((D, units), BF),
            jax.ShapeDtypeStruct((D, units), BF),
            jax.ShapeDtypeStruct((units, D), BF),
        ],
        input_output_aliases={5 + k: k for k in range(len(before))},
        compiler_params=pltpu.CompilerParams(vmem_limit_bytes=60 * 1024 * 1024),
        name="other_grads" if flip else "own_grads",
    )(core, rows, rows, hidden_t, cots, *before)


def combine_kernel(target, rows, out):
    tokens = target.shape[0]
    row = lax.broadcasted_iota(jnp.int32, (tokens, rows.shape[0]), 1)
    hit = (row == target[:, 0:1]) | (row == target[:, 1:2])
    select = jnp.where(hit, 1.0, 0.0).astype(BF)
    width = out.shape[2]
    for pair in range(out.shape[0] // 2):
        both = jnp.dot(
            select,
            rows[:, 2 * pair * width : 2 * (pair + 1) * width],
            preferred_element_type=F32,
        ).astype(BF)
        out[2 * pair] = both[:, :width]
        out[2 * pair + 1] = both[:, width:]


def combined(target, rows):
    tokens = target.shape[0]
    cols = 128
    return pl.pallas_call(
        combine_kernel,
        in_specs=in_vmem(2),
        out_specs=in_vmem(1)[0],
        out_shape=jax.ShapeDtypeStruct((rows.shape[1] // cols, tokens, cols), BF),
        compiler_params=small_vmem(),
        name="combine",
    )(target, rows)


def mix_kernel(place, pieces, cotangent, out):
    mixed = cotangent[...].astype(F32)
    for k in range(pieces.shape[0]):
        mixed = mixed + pieces[k].astype(F32)
    for k in range(out.shape[0]):
        out[k] = mixed.astype(BF)


def mixed_copies(place, pieces, cotangent):
    depth, tokens, share = pieces.shape
    return pl.pallas_call(
        mix_kernel,
        grid_spec=pltpu.PrefetchScalarGridSpec(
            num_scalar_prefetch=1,
            grid=(1,),
            in_specs=in_vmem(1) + [pl.BlockSpec((tokens, share), lambda i, p: (0, p[0]))],
            out_specs=in_vmem(1)[0],
        ),
        out_shape=jax.ShapeDtypeStruct((depth, tokens, share), BF),
        compiler_params=small_vmem(),
        name="mix",
    )(place, pieces, cotangent)


def normalised(conv_out, mean, rstd, gain):
    centered = (conv_out[...].astype(F32) - mean[...]) * rstd[...]
    channels = conv_out.shape[0]
    column = jnp.broadcast_to(gain[...], (channels, channels)).T
    wide = jnp.concatenate([column] * (conv_out.shape[1] // channels), axis=1)
    return centered, centered * wide, wide


def norm_kernel(core, mixed_own, mixed_other, w_out, conv_out, mean, rstd, gain, norm_cot, sums):
    depth, tokens, share = mixed_own.shape
    turned = jnp.zeros((tokens, w_out.shape[1]), F32)
    for flip, mixed in ((False, mixed_own), (True, mixed_other)):
        base = (1 - core[0] if flip else core[0]) * HALF
        for k in range(depth):
            rows = pl.ds(pl.multiple_of(base + k * share, share), share)
            turned = turned + contract(mixed[k], w_out[rows, :], 1, 0)
    centered, normed, wide = normalised(conv_out, mean, rstd, gain)
    sigma = jax.nn.sigmoid(normed)
    cot = turned.T * sigma * (1.0 + normed * (1.0 - sigma)) * wide
    norm_cot[...] = cot
    first = jnp.sum(cot, axis=0, keepdims=True)
    second = jnp.sum(cot * centered, axis=0, keepdims=True)
    for k in range(sums.shape[0]):
        sums[k, 0:1, :] = first
        sums[k, 1:2, :] = second


def norm_cotangent(core, mixed_own, mixed_other, w_out, conv_out, mean, rstd, gain, copies):
    channels, tokens = conv_out.shape
    return pl.pallas_call(
        norm_kernel,
        in_specs=[SCALAR] + in_vmem(7),
        out_specs=in_vmem(2),
        out_shape=[
            jax.ShapeDtypeStruct((channels, tokens), F32),
            jax.ShapeDtypeStruct((copies, 2, tokens), F32),
        ],
        compiler_params=small_vmem(),
        name="norm_cot",
    )(core, mixed_own, mixed_other, w_out, conv_out, mean, rstd, gain)


def proj_kernel(core, mixed_own, mixed_other, conv_out, mean, rstd, gain, out):
    depth = mixed_own.shape[0]
    _, normed, _ = normalised(conv_out, mean, rstd, gain)
    act = (normed * jax.nn.sigmoid(normed)).astype(BF)
    for flip, mixed in ((False, mixed_own), (True, mixed_other)):
        base = (1 - core[0] if flip else core[0]) * depth
        for k in range(depth):
            out[base + k] = contract(act, mixed[k], 1, 0).astype(BF)


def proj_parts(core, mixed_own, mixed_other, conv_out, mean, rstd, gain):
    depth, _, share = mixed_own.shape
    return pl.pallas_call(
        proj_kernel,
        in_specs=[SCALAR] + in_vmem(6),
        out_specs=in_vmem(1)[0],
        out_shape=jax.ShapeDtypeStruct((2 * depth, conv_out.shape[0], share), BF),
        compiler_params=small_vmem(),
        name="proj_parts",
    )(core, mixed_own, mixed_other, conv_out, mean, rstd, gain)


RIM = 32


def conv_cot_kernel(sums, norm_cot, conv_out, mean, rstd, turned, rim):
    total = sums[0]
    for k in range(1, sums.shape[0]):
        total = total + sums[k]
    centered = (conv_out[...].astype(F32) - mean[...]) * rstd[...]
    cot = rstd[...] * (norm_cot[...] - total[0:1, :] / C - centered * (total[1:2, :] / C))
    across = cot.T
    turned[...] = across
    rim[...] = across[:RIM, :]


def conv_cotangent(sums, norm_cot, conv_out, mean, rstd):
    channels, tokens = conv_out.shape
    return pl.pallas_call(
        conv_cot_kernel,
        in_specs=in_vmem(5),
        out_specs=in_vmem(2),
        out_shape=[
            jax.ShapeDtypeStruct((tokens, channels), F32),
            jax.ShapeDtypeStruct((RIM, channels), F32),
        ],
        compiler_params=small_vmem(),
        name="conv_cot",
    )(sums, norm_cot, conv_out, mean, rstd)


def glu_kernel(turned, rim, taps, glu_value, glu_gate, value_grad, gate_grad, padded):
    tokens = turned.shape[0]
    padded[:tokens, :] = turned[...]
    padded[tokens:, :] = rim[...]
    total = taps[0:1, :] * turned[...]
    for lag in range(1, taps.shape[0]):
        total = total + taps[lag : lag + 1, :] * padded[lag : lag + tokens, :]
    cot = total.T
    sigma = jax.nn.sigmoid(glu_gate[...].astype(F32))
    value_grad[...] = (cot * sigma).astype(BF)
    gate_grad[...] = (cot * glu_value[...].astype(F32) * sigma * (1.0 - sigma)).astype(BF)


def glu_cotangents(turned, rim, taps, glu_value, glu_gate):
    tokens, channels = turned.shape
    return pl.pallas_call(
        glu_kernel,
        in_specs=in_vmem(5),
        out_specs=in_vmem(2),
        out_shape=[jax.ShapeDtypeStruct((channels, tokens), BF)] * 2,
        scratch_shapes=[pltpu.VMEM((tokens + RIM, channels), F32)],
        compiler_params=small_vmem(),
        name="glu_cot",
    )(turned, rim, taps, glu_value, glu_gate)


def proj_sum_kernel(parts, out):
    total = parts[0].astype(F32)
    for k in range(1, parts.shape[0]):
        total = total + parts[k].astype(F32)
    out[...] = total.T


def proj_summed(parts):
    return pl.pallas_call(
        proj_sum_kernel,
        in_specs=in_vmem(1),
        out_specs=in_vmem(1)[0],
        out_shape=jax.ShapeDtypeStruct((parts.shape[2], parts.shape[1]), F32),
        compiler_params=small_vmem(),
        name="proj_sum",
    )(parts)


def on_device(
    saved_input,
    cotangent,
    expert_ids,
    route_weight,
    w_gate,
    w_up,
    w_down,
    w_out,
    channel_gain,
    conv_taps,
    glu_value,
    glu_gate,
    conv_out,
    norm_mean,
    norm_rstd,
):
    tokens = cotangent.shape[0]
    sp_count = lax.axis_size("sp")
    experts = sp_count
    slots = 4 * tokens // experts
    tp_index = lax.axis_index("tp").astype(jnp.int32)
    core_index = tp_index & 1
    tp_count = lax.axis_size("tp")
    depth = tp_count // 2
    same_core = [[2 * z + c for z in range(depth)] for c in range(2)]
    core = core_index.reshape(1)
    place = (core_index * depth + (tp_index >> 1)).reshape(1)
    pairs = jnp.concatenate([expert_ids.astype(F32), route_weight], axis=1).T
    mine = core_index * HALF
    half_in = lax.dynamic_slice(saved_input, (0, mine), (tokens, HALF))
    half_cot = lax.dynamic_slice(cotangent, (0, mine), (tokens, HALF))
    core, place, pairs = lax.optimization_barrier((core, place, pairs))

    sent, target = routed(pairs, half_in, half_cot, experts, slots)
    own = exchanged(sent.reshape(experts, slots, D), "sp").reshape(sp_count * slots, D)
    other = swapped_cores(own)
    gate_w, up_w, down_w = w_gate[0], w_up[0], w_down[0]
    first_part, cot_part, pair_own, pair_other = own_products(core, own, gate_w, up_w, down_w)
    hidden, cots, send = other_products(core, other, first_part, cot_part, pair_other, down_w)
    received = swapped_cores(send)
    keep, hidden_t = kept_half(cots, pair_own, hidden)
    input_cot = pair_sum(keep, received)
    returned = exchanged(input_cot.reshape(sp_count, slots, HALF), "sp")

    partial = combined(target, returned.reshape(experts * slots, HALF))
    pieces = exchanged(partial, "tp", same_core)
    copies = mixed_copies(place, pieces, cotangent)
    mixed_own = exchanged(copies, "tp", same_core)
    mixed_other = swapped_cores(mixed_own)

    mixed_other, late_own, late_other, late_cots, late_hidden = lax.optimization_barrier(
        (mixed_other, own, other, cots, hidden_t)
    )
    mean, rstd = norm_mean.reshape(1, tokens), norm_rstd.reshape(1, tokens)
    gain = channel_gain.reshape(1, -1)
    norm_cot, sums = norm_cotangent(
        core, mixed_own, mixed_other, w_out, conv_out, mean, rstd, gain, tp_count
    )
    all_sums = exchanged(sums, "tp")
    proj_part = proj_parts(core, mixed_own, mixed_other, conv_out, mean, rstd, gain)
    proj_pieces = exchanged(proj_part, "sp")
    proj_grad = proj_summed(proj_pieces)
    half_done = half_grads(core, False, late_own, late_hidden, late_cots)
    all_sums, *half_done = lax.optimization_barrier((all_sums, *half_done))
    turned, rim = conv_cotangent(all_sums, norm_cot, conv_out, mean, rstd)
    rim = lax.ppermute(rim, "sp", [(i, i - 1) for i in range(1, sp_count)])
    turned, late_other = lax.optimization_barrier((turned, late_other))
    gate_grad, up_grad, down_grad = half_grads(
        core, True, late_other, late_hidden, late_cots, half_done
    )
    value_grad, gate_in_grad = glu_cotangents(turned, rim, conv_taps, glu_value, glu_gate)
    return (
        gate_grad[None],
        up_grad[None],
        down_grad[None],
        proj_grad,
        value_grad,
        gate_in_grad,
    )


def solution(mesh):
    in_specs = (
        P("sp", None),
        P("sp", None),
        P("sp", None),
        P("sp", None),
        P("sp", None, "tp"),
        P("sp", None, "tp"),
        P("sp", "tp", None),
        P(None, "tp"),
        P("tp"),
        P(None, "tp"),
        P("tp", "sp"),
        P("tp", "sp"),
        P("tp", "sp"),
        P("sp"),
        P("sp"),
    )
    out_specs = (
        P("sp", None, "tp"),
        P("sp", None, "tp"),
        P("sp", "tp", None),
        P("sp", "tp"),
        P("tp", "sp"),
        P("tp", "sp"),
    )
    return jax.shard_map(
        on_device, mesh=mesh, in_specs=in_specs, out_specs=out_specs, check_vma=False
    )
```

```python
import functools

import jax
import jax.numpy as jnp
from jax import lax
from jax.experimental import pallas as pl
from jax.experimental.pallas import tpu as pltpu
from jax.sharding import PartitionSpec as P


D = 2048
C = 2048
HALF = D // 2
BF = jnp.bfloat16
F32 = jnp.float32


def contract(left, right, left_dim, right_dim):
    return lax.dot_general(
        left, right, (((left_dim,), (right_dim,)), ((), ())), preferred_element_type=F32
    )


def exchanged(value, axis, groups=None):
    return lax.all_to_all(value, axis, 0, 0, axis_index_groups=groups, tiled=True)


def swapped_cores(value):
    pairs = [(i, i ^ 1) for i in range(lax.axis_size("tp"))]
    return lax.ppermute(value, "tp", pairs)


def small_vmem():
    return pltpu.CompilerParams(vmem_limit_bytes=6 * 1024 * 1024)


def in_vmem(count):
    return [pl.BlockSpec(memory_space=pltpu.VMEM)] * count


SCALAR = pl.BlockSpec(memory_space=pltpu.SMEM)


def route_kernel(pairs, saved_input, cotangent, sent, target, *, experts, slots):
    tokens = pairs.shape[1]
    ids = pairs[0:2, :].astype(jnp.int32)
    weights = pairs[2:4, :]
    expert = lax.broadcasted_iota(jnp.int32, (experts, tokens), 0)
    first = ids[0:1, :] == expert
    second = ids[1:2, :] == expert
    named = jnp.where(first | second, 1.0, 0.0).astype(BF)
    earlier = lax.broadcasted_iota(jnp.int32, (tokens, tokens), 0) < lax.broadcasted_iota(
        jnp.int32, (tokens, tokens), 1
    )
    count = jnp.dot(named, jnp.where(earlier, 1.0, 0.0).astype(BF), preferred_element_type=F32)
    places = []
    for k, chosen in ((0, first), (1, second)):
        slot = jnp.sum(jnp.where(chosen, count, 0.0), axis=0, keepdims=True)
        places.append(ids[k : k + 1, :] * slots + slot.astype(jnp.int32))
    across = jnp.concatenate(places + [jnp.zeros((6, tokens), jnp.int32)], axis=0)
    target[...] = across.astype(F32).T[:, 0:2].astype(jnp.int32)

    rows = 256
    for step in range(experts * slots // rows):
        row = lax.broadcasted_iota(jnp.int32, (rows, tokens), 0) + step * rows
        hit0 = row == places[0]
        hit1 = row == places[1]
        select = jnp.where(hit0 | hit1, 1.0, 0.0).astype(BF)
        weight = jnp.sum(
            jnp.where(hit0, weights[0:1, :], 0.0) + jnp.where(hit1, weights[1:2, :], 0.0),
            axis=1,
            keepdims=True,
        )
        here = slice(step * rows, (step + 1) * rows)
        moved_in = jnp.dot(select, saved_input[...], preferred_element_type=F32)
        sent[here, :HALF] = moved_in.astype(BF)
        moved = jnp.dot(select, cotangent[...], preferred_element_type=F32)
        sent[here, HALF:] = (moved * weight).astype(BF)


def routed(pairs, half_in, half_cot, experts, slots):
    tokens = pairs.shape[1]
    return pl.pallas_call(
        functools.partial(route_kernel, experts=experts, slots=slots),
        in_specs=in_vmem(3),
        out_specs=in_vmem(2),
        out_shape=[
            jax.ShapeDtypeStruct((experts * slots, D), BF),
            jax.ShapeDtypeStruct((tokens, 2), jnp.int32),
        ],
        compiler_params=small_vmem(),
        name="route",
    )(pairs, half_in, half_cot)


ROWS = 256


def half_of(core, flip):
    index = 1 - core[0] if flip else core[0]
    return pl.ds(pl.multiple_of(index * HALF, HALF), HALF)


def own_kernel(
    core, own, w_gate, w_up, w_down, first_part, cot_part, own_t, pair_other, other_t, down_t,
    pair_own,
):
    units = w_gate.shape[1]
    half, far = half_of(core, False), half_of(core, True)
    pair_own[:, :units] = w_gate[half, :]
    pair_own[:, units:] = w_up[half, :]
    for step in range(own.shape[0] // ROWS):
        here = slice(step * ROWS, (step + 1) * ROWS)
        first_part[here, :] = contract(own[here, :HALF], pair_own[...], 1, 0)
        cot_part[here, :] = contract(own[here, HALF:], w_down[:, half], 1, 1)
    pair_other[:, :units] = w_gate[far, :]
    pair_other[:, units:] = w_up[far, :]
    down_t[...] = w_down[:, far].T
    other_t[...] = pair_other[...].T
    own_t[...] = pair_own[...].T


def own_products(core, own, w_gate, w_up, w_down):
    total, units = own.shape[0], w_gate.shape[1]
    return pl.pallas_call(
        own_kernel,
        in_specs=[SCALAR] + in_vmem(4),
        out_specs=in_vmem(6),
        out_shape=[
            jax.ShapeDtypeStruct((total, 2 * units), F32),
            jax.ShapeDtypeStruct((total, units), F32),
            jax.ShapeDtypeStruct((2 * units, HALF), BF),
            jax.ShapeDtypeStruct((HALF, 2 * units), BF),
            jax.ShapeDtypeStruct((2 * units, HALF), BF),
            jax.ShapeDtypeStruct((HALF, units), BF),
        ],
        scratch_shapes=[pltpu.VMEM((HALF, 2 * units), BF)],
        compiler_params=small_vmem(),
        name="own_products",
    )(core, own, w_gate, w_up, w_down)


def other_kernel(
    other, first_part, cot_part, pair_other, other_t, down_t, hidden, cots, send,
):
    units = down_t.shape[1]
    for step in range(other.shape[0] // ROWS):
        here = slice(step * ROWS, (step + 1) * ROWS)
        first = first_part[here, :] + contract(other[here, :HALF], pair_other[...], 1, 0)
        gate_pre, up_pre = first[:, :units], first[:, units:]
        hidden_cot = cot_part[here, :] + contract(other[here, HALF:], down_t[...], 1, 0)
        sigma = jax.nn.sigmoid(gate_pre)
        silu = gate_pre * sigma
        hidden[here, :] = (silu * up_pre).astype(BF)
        cots[here, :units] = (
            hidden_cot * up_pre * sigma * (1.0 + gate_pre * (1.0 - sigma))
        ).astype(BF)
        cots[here, units:] = (hidden_cot * silu).astype(BF)
        send[here, :] = contract(cots[here, :], other_t[...], 1, 0).astype(BF)


def other_products(other, first_part, cot_part, pair_other, other_t, down_t):
    total, units = other.shape[0], down_t.shape[1]
    return pl.pallas_call(
        other_kernel,
        in_specs=in_vmem(6),
        out_specs=in_vmem(3),
        out_shape=[
            jax.ShapeDtypeStruct((total, units), BF),
            jax.ShapeDtypeStruct((total, 2 * units), BF),
            jax.ShapeDtypeStruct((total, HALF), BF),
        ],
        compiler_params=small_vmem(),
        name="other_products",
    )(other, first_part, cot_part, pair_other, other_t, down_t)


def keep_kernel(cots, own_t, hidden, keep, hidden_t):
    for step in range(keep.shape[0] // ROWS):
        here = slice(step * ROWS, (step + 1) * ROWS)
        keep[here, :] = contract(cots[here, :], own_t[...], 1, 0).astype(BF)
    hidden_t[...] = hidden[...].T


def kept_half(cots, own_t, hidden):
    total, units = hidden.shape
    return pl.pallas_call(
        keep_kernel,
        in_specs=in_vmem(3),
        out_specs=in_vmem(2),
        out_shape=[
            jax.ShapeDtypeStruct((total, HALF), BF),
            jax.ShapeDtypeStruct((units, total), BF),
        ],
        compiler_params=small_vmem(),
        name="kept_half",
    )(cots, own_t, hidden)


def sum_kernel(keep, received, out):
    out[...] = (keep[...].astype(F32) + received[...].astype(F32)).astype(BF)


def pair_sum(keep, received):
    return pl.pallas_call(
        sum_kernel,
        in_specs=in_vmem(2),
        out_specs=in_vmem(1)[0],
        out_shape=jax.ShapeDtypeStruct(keep.shape, BF),
        compiler_params=small_vmem(),
        name="pair_sum",
    )(keep, received)


def grad_kernel(core, rows_in, rows_cot, hidden_t, cots, *rest):
    gate_grad, up_grad, down_grad = rest[-3:]
    units = gate_grad.shape[1]
    both = contract(rows_in[...].T, cots[...], 1, 0).astype(BF)
    gate_grad[...] = both[:, :units]
    up_grad[...] = both[:, units:]
    down_grad[...] = contract(hidden_t[...], rows_cot[...], 1, 0).astype(BF)


def half_grads(core, flip, rows, hidden_t, cots, before=()):
    units, total = hidden_t.shape
    cols = 256
    steps = HALF // cols

    def place(i, c):
        return (1 - c[0] if flip else c[0]) * steps + i

    return pl.pallas_call(
        grad_kernel,
        grid_spec=pltpu.PrefetchScalarGridSpec(
            num_scalar_prefetch=1,
            grid=(steps,),
            in_specs=[
                pl.BlockSpec((total, cols), lambda i, c: (0, i)),
                pl.BlockSpec((total, cols), lambda i, c: (0, i + steps)),
                pl.BlockSpec((units, total), lambda i, c: (0, 0)),
                pl.BlockSpec((total, 2 * units), lambda i, c: (0, 0)),
            ]
            + [pl.BlockSpec(memory_space=pl.ANY)] * len(before),
            out_specs=[
                pl.BlockSpec((cols, units), lambda i, c: (place(i, c), 0)),
                pl.BlockSpec((cols, units), lambda i, c: (place(i, c), 0)),
                pl.BlockSpec((units, cols), lambda i, c: (0, place(i, c))),
            ],
        ),
        out_shape=[
            jax.ShapeDtypeStruct((D, units), BF),
            jax.ShapeDtypeStruct((D, units), BF),
            jax.ShapeDtypeStruct((units, D), BF),
        ],
        input_output_aliases={5 + k: k for k in range(len(before))},
        compiler_params=pltpu.CompilerParams(vmem_limit_bytes=60 * 1024 * 1024),
        name="other_grads" if flip else "own_grads",
    )(core, rows, rows, hidden_t, cots, *before)


def combine_kernel(target, rows, out):
    tokens = target.shape[0]
    row = lax.broadcasted_iota(jnp.int32, (tokens, rows.shape[0]), 1)
    hit = (row == target[:, 0:1]) | (row == target[:, 1:2])
    select = jnp.where(hit, 1.0, 0.0).astype(BF)
    width = out.shape[2]
    for pair in range(out.shape[0] // 2):
        both = jnp.dot(
            select,
            rows[:, 2 * pair * width : 2 * (pair + 1) * width],
            preferred_element_type=F32,
        ).astype(BF)
        out[2 * pair] = both[:, :width]
        out[2 * pair + 1] = both[:, width:]


def combined(target, rows):
    tokens = target.shape[0]
    cols = 128
    return pl.pallas_call(
        combine_kernel,
        in_specs=in_vmem(2),
        out_specs=in_vmem(1)[0],
        out_shape=jax.ShapeDtypeStruct((rows.shape[1] // cols, tokens, cols), BF),
        compiler_params=small_vmem(),
        name="combine",
    )(target, rows)


def mix_kernel(place, pieces, cotangent, out):
    mixed = cotangent[...].astype(F32)
    for k in range(pieces.shape[0]):
        mixed = mixed + pieces[k].astype(F32)
    for k in range(out.shape[0]):
        out[k] = mixed.astype(BF)


def mixed_copies(place, pieces, cotangent):
    depth, tokens, share = pieces.shape
    return pl.pallas_call(
        mix_kernel,
        grid_spec=pltpu.PrefetchScalarGridSpec(
            num_scalar_prefetch=1,
            grid=(1,),
            in_specs=in_vmem(1) + [pl.BlockSpec((tokens, share), lambda i, p: (0, p[0]))],
            out_specs=in_vmem(1)[0],
        ),
        out_shape=jax.ShapeDtypeStruct((depth, tokens, share), BF),
        compiler_params=small_vmem(),
        name="mix",
    )(place, pieces, cotangent)


def normalised(conv_out, mean, rstd, gain):
    centered = (conv_out[...].astype(F32) - mean[...]) * rstd[...]
    channels = conv_out.shape[0]
    column = jnp.broadcast_to(gain[...], (channels, channels)).T
    wide = jnp.concatenate([column] * (conv_out.shape[1] // channels), axis=1)
    return centered, centered * wide, wide


def mixed_kernel(core, mixed, w_out, conv_out, mean, rstd, gain, turned, parts):
    depth, tokens, share = mixed.shape
    _, normed, _ = normalised(conv_out, mean, rstd, gain)
    act = (normed * jax.nn.sigmoid(normed)).astype(BF)
    total = jnp.zeros((tokens, w_out.shape[1]), F32)
    for k in range(depth):
        rows = pl.ds(pl.multiple_of(core[0] * HALF + k * share, share), share)
        total = total + contract(mixed[k], w_out[rows, :], 1, 0)
        parts[k] = contract(act, mixed[k], 1, 0).astype(BF)
    turned[...] = total


def own_mixed_products(core, mixed, w_out, conv_out, mean, rstd, gain):
    depth, tokens, share = mixed.shape
    channels = w_out.shape[1]
    return pl.pallas_call(
        mixed_kernel,
        in_specs=[SCALAR] + in_vmem(6),
        out_specs=in_vmem(2),
        out_shape=[
            jax.ShapeDtypeStruct((tokens, channels), F32),
            jax.ShapeDtypeStruct((depth, channels, share), BF),
        ],
        compiler_params=small_vmem(),
        name="own_mixed",
    )(core, mixed, w_out, conv_out, mean, rstd, gain)


def norm_kernel(core, mixed, turned_part, w_out, conv_out, mean, rstd, gain, norm_cot, sums):
    depth, _, share = mixed.shape
    turned = turned_part[...]
    base = (1 - core[0]) * HALF
    for k in range(depth):
        rows = pl.ds(pl.multiple_of(base + k * share, share), share)
        turned = turned + contract(mixed[k], w_out[rows, :], 1, 0)
    centered, normed, wide = normalised(conv_out, mean, rstd, gain)
    sigma = jax.nn.sigmoid(normed)
    cot = turned.T * sigma * (1.0 + normed * (1.0 - sigma)) * wide
    norm_cot[...] = cot
    first = jnp.sum(cot, axis=0, keepdims=True)
    second = jnp.sum(cot * centered, axis=0, keepdims=True)
    both = jnp.concatenate([first, second], axis=0)
    for k in range(sums.shape[0]):
        sums[k] = both


def norm_cotangent(core, mixed, turned_part, w_out, conv_out, mean, rstd, gain, copies):
    channels, tokens = conv_out.shape
    return pl.pallas_call(
        norm_kernel,
        in_specs=[SCALAR] + in_vmem(7),
        out_specs=in_vmem(2),
        out_shape=[
            jax.ShapeDtypeStruct((channels, tokens), F32),
            jax.ShapeDtypeStruct((copies, 2, tokens), F32),
        ],
        compiler_params=small_vmem(),
        name="norm_cot",
    )(core, mixed, turned_part, w_out, conv_out, mean, rstd, gain)


def proj_kernel(core, mixed, own_parts, conv_out, mean, rstd, gain, out):
    depth = mixed.shape[0]
    _, normed, _ = normalised(conv_out, mean, rstd, gain)
    act = (normed * jax.nn.sigmoid(normed)).astype(BF)
    for k in range(depth):
        out[core[0] * depth + k] = own_parts[k]
        out[(1 - core[0]) * depth + k] = contract(act, mixed[k], 1, 0).astype(BF)


def proj_parts(core, mixed, own_parts, conv_out, mean, rstd, gain):
    depth, channels, share = own_parts.shape
    return pl.pallas_call(
        proj_kernel,
        in_specs=[SCALAR] + in_vmem(6),
        out_specs=in_vmem(1)[0],
        out_shape=jax.ShapeDtypeStruct((2 * depth, channels, share), BF),
        compiler_params=small_vmem(),
        name="proj_parts",
    )(core, mixed, own_parts, conv_out, mean, rstd, gain)


RIM = 32


def conv_cot_kernel(sums, norm_cot, conv_out, mean, rstd, turned, rim):
    total = sums[0]
    for k in range(1, sums.shape[0]):
        total = total + sums[k]
    centered = (conv_out[...].astype(F32) - mean[...]) * rstd[...]
    cot = rstd[...] * (norm_cot[...] - total[0:1, :] / C - centered * (total[1:2, :] / C))
    across = cot.T
    turned[...] = across
    rim[...] = across[:RIM, :]


def conv_cotangent(sums, norm_cot, conv_out, mean, rstd):
    channels, tokens = conv_out.shape
    return pl.pallas_call(
        conv_cot_kernel,
        in_specs=in_vmem(5),
        out_specs=in_vmem(2),
        out_shape=[
            jax.ShapeDtypeStruct((tokens, channels), F32),
            jax.ShapeDtypeStruct((RIM, channels), F32),
        ],
        compiler_params=small_vmem(),
        name="conv_cot",
    )(sums, norm_cot, conv_out, mean, rstd)


def glu_kernel(turned, rim, taps, glu_value, glu_gate, value_grad, gate_grad, padded):
    tokens = turned.shape[0]
    padded[:tokens, :] = turned[...]
    padded[tokens:, :] = rim[...]
    total = taps[0:1, :] * turned[...]
    for lag in range(1, taps.shape[0]):
        total = total + taps[lag : lag + 1, :] * padded[lag : lag + tokens, :]
    cot = total.T
    sigma = jax.nn.sigmoid(glu_gate[...].astype(F32))
    value_grad[...] = (cot * sigma).astype(BF)
    gate_grad[...] = (cot * glu_value[...].astype(F32) * sigma * (1.0 - sigma)).astype(BF)


def glu_cotangents(turned, rim, taps, glu_value, glu_gate):
    tokens, channels = turned.shape
    return pl.pallas_call(
        glu_kernel,
        in_specs=in_vmem(5),
        out_specs=in_vmem(2),
        out_shape=[jax.ShapeDtypeStruct((channels, tokens), BF)] * 2,
        scratch_shapes=[pltpu.VMEM((tokens + RIM, channels), F32)],
        compiler_params=small_vmem(),
        name="glu_cot",
    )(turned, rim, taps, glu_value, glu_gate)


def proj_sum_kernel(parts, out):
    total = parts[0].astype(F32)
    for k in range(1, parts.shape[0]):
        total = total + parts[k].astype(F32)
    out[...] = total.T


def proj_summed(parts):
    return pl.pallas_call(
        proj_sum_kernel,
        in_specs=in_vmem(1),
        out_specs=in_vmem(1)[0],
        out_shape=jax.ShapeDtypeStruct((parts.shape[2], parts.shape[1]), F32),
        compiler_params=small_vmem(),
        name="proj_sum",
    )(parts)


def on_device(
    saved_input,
    cotangent,
    expert_ids,
    route_weight,
    w_gate,
    w_up,
    w_down,
    w_out,
    channel_gain,
    conv_taps,
    glu_value,
    glu_gate,
    conv_out,
    norm_mean,
    norm_rstd,
):
    tokens = cotangent.shape[0]
    sp_count = lax.axis_size("sp")
    experts = sp_count
    slots = 4 * tokens // experts
    tp_index = lax.axis_index("tp").astype(jnp.int32)
    core_index = tp_index & 1
    tp_count = lax.axis_size("tp")
    depth = tp_count // 2
    same_core = [[2 * z + c for z in range(depth)] for c in range(2)]
    core = core_index.reshape(1)
    place = (core_index * depth + (tp_index >> 1)).reshape(1)
    pairs = jnp.concatenate([expert_ids.astype(F32), route_weight], axis=1).T
    mine = core_index * HALF
    half_in = lax.dynamic_slice(saved_input, (0, mine), (tokens, HALF))
    half_cot = lax.dynamic_slice(cotangent, (0, mine), (tokens, HALF))
    core, place, pairs = lax.optimization_barrier((core, place, pairs))

    sent, target = routed(pairs, half_in, half_cot, experts, slots)
    own = exchanged(sent.reshape(experts, slots, D), "sp").reshape(sp_count * slots, D)
    other = swapped_cores(own)
    gate_w, up_w, down_w = w_gate[0], w_up[0], w_down[0]
    first_part, cot_part, own_t, pair_other, other_t, down_t = own_products(
        core, own, gate_w, up_w, down_w
    )
    hidden, cots, send = other_products(other, first_part, cot_part, pair_other, other_t, down_t)
    received = swapped_cores(send)
    keep, hidden_t = kept_half(cots, own_t, hidden)
    input_cot = pair_sum(keep, received)
    returned = exchanged(input_cot.reshape(sp_count, slots, HALF), "sp")

    partial = combined(target, returned.reshape(experts * slots, HALF))
    pieces = exchanged(partial, "tp", same_core)
    copies = mixed_copies(place, pieces, cotangent)
    mixed_own = exchanged(copies, "tp", same_core)
    mixed_other = swapped_cores(mixed_own)
    mean, rstd = norm_mean.reshape(1, tokens), norm_rstd.reshape(1, tokens)
    gain = channel_gain.reshape(1, -1)
    turned_part, own_parts = own_mixed_products(
        core, mixed_own, w_out, conv_out, mean, rstd, gain
    )
    norm_cot, sums = norm_cotangent(
        core, mixed_other, turned_part, w_out, conv_out, mean, rstd, gain, tp_count
    )
    all_sums = exchanged(sums, "tp")
    proj_part = proj_parts(core, mixed_other, own_parts, conv_out, mean, rstd, gain)
    proj_pieces = exchanged(proj_part, "sp")
    proj_grad = proj_summed(proj_pieces)
    mixed_other, late_own, late_other, late_cots, late_hidden = lax.optimization_barrier(
        (mixed_other, own, other, cots, hidden_t)
    )
    half_done = half_grads(core, False, late_own, late_hidden, late_cots)
    all_sums, *half_done = lax.optimization_barrier((all_sums, *half_done))
    turned, rim = conv_cotangent(all_sums, norm_cot, conv_out, mean, rstd)
    rim = lax.ppermute(rim, "sp", [(i, i - 1) for i in range(1, sp_count)])
    turned, late_other = lax.optimization_barrier((turned, late_other))
    gate_grad, up_grad, down_grad = half_grads(
        core, True, late_other, late_hidden, late_cots, half_done
    )
    value_grad, gate_in_grad = glu_cotangents(turned, rim, conv_taps, glu_value, glu_gate)
    return (
        gate_grad[None],
        up_grad[None],
        down_grad[None],
        proj_grad,
        value_grad,
        gate_in_grad,
    )


def solution(mesh):
    in_specs = (
        P("sp", None),
        P("sp", None),
        P("sp", None),
        P("sp", None),
        P("sp", None, "tp"),
        P("sp", None, "tp"),
        P("sp", "tp", None),
        P(None, "tp"),
        P("tp"),
        P(None, "tp"),
        P("tp", "sp"),
        P("tp", "sp"),
        P("tp", "sp"),
        P("sp"),
        P("sp"),
    )
    out_specs = (
        P("sp", None, "tp"),
        P("sp", None, "tp"),
        P("sp", "tp", None),
        P("sp", "tp"),
        P("tp", "sp"),
        P("tp", "sp"),
    )
    return jax.shard_map(
        on_device, mesh=mesh, in_specs=in_specs, out_specs=out_specs, check_vma=False
    )
```
